32 devices in a mesh: sp: 16 (over z, y, x), tp: 2 (over core).
Axes of the slice: x: 2, y: 2, z: 4, core: 2. Of those that a mesh axis runs over, the one named last changes fastest.
Arguments:
- latent: bfloat16 [4096, 2048], P(('sp', 'tp')), may hold values from -6 to 6
- cond: float32 [2048], replicated, may hold values from -6 to 6
- ctx_mod: float32 [2048], replicated, may hold values from -6 to 6
- context: bfloat16 [512, 2048], P(('sp', 'tp')), may hold values from -6 to 6
- shift_w: float32 [2048, 2048], P('sp', 'tp'), may hold values from -0.125 to 0.125
- scale_w: float32 [2048, 2048], P('sp', 'tp'), may hold values from -0.125 to 0.125
- gate_w: float32 [2048, 2048], P('sp', 'tp'), may hold values from -0.125 to 0.125
- norm_gain: float32 [2048], replicated, may hold values from 0.1 to 1.9
- w_qn: bfloat16 [2048, 2048], P(None, 'tp'), may hold values from -0.125 to 0.125
- w_qr: bfloat16 [2048, 1024], P(None, 'tp'), may hold values from -0.13258252 to 0.13258252
- w_kv_down: bfloat16 [2048, 512], replicated, may hold values from -0.125 to 0.125
- w_rope_key: bfloat16 [2048, 64], replicated, may hold values from -0.13258252 to 0.13258252
- kv_gain: float32 [512], replicated, may hold values from 0.1 to 1.9
- w_key_up: bfloat16 [512, 2048], P(None, 'tp'), may hold values from -0.66015625 to 0.66015625
- w_value_up: bfloat16 [512, 2048], P(None, 'tp'), may hold values from -0.25 to 0.25
- ctx_bias: float32 [16], P('tp'), may hold values from 2 to 3.5
- w_out: bfloat16 [2048, 2048], P('tp'), may hold values from -0.52734375 to 0.52734375
Outputs:
- mixed: bfloat16 [4096, 2048], P(('sp', 'tp'))
The draws below stay inside these ranges and needn't reach their ends.
All inputs are finite; a program needn't handle non-finite values.
Results may differ from the reference program's by a relative error of at most 0.018.
Values may be sent and summed in bfloat16 or wider, within the bound.
A program may use at most 128 MiB of HBM per device.

```python
import jax
import jax.numpy as jnp
from jax import lax

D = 2048
HEADS = 16
NOPE = 128
ROPE = 64
VDIM = 128
KV_RANK = 512
GRID_W = 128
CTX = 512
SEQ = 4096
HEADS_DEV = 8
N_TP = 2


def weight_base(key, shape):
    return jax.random.normal(key, shape, jnp.float32) * D ** (-0.5)


def draw_latent(key, part):
    tokens = jax.random.normal(jax.random.fold_in(key, 1), (SEQ, D), jnp.float32)
    return jnp.clip(tokens, -6.0, 6.0).astype(jnp.bfloat16)


def draw_w_qr(key, part):
    matrix = weight_base(jax.random.fold_in(key, 5), (D, HEADS * ROPE))
    bound = 6.0 * D ** (-0.5)
    return jnp.clip(matrix, -bound, bound).astype(jnp.bfloat16)


def draw_w_rope_key(key, part):
    matrix = weight_base(jax.random.fold_in(key, 6), (D, ROPE))
    bound = 6.0 * D ** (-0.5)
    return jnp.clip(matrix, -bound, bound).astype(jnp.bfloat16)


def steps_of(own_key, shape, cuts, smallest, largest):
    loudness = 1.0
    for position, shards_of in cuts:
        steps = jax.random.uniform(jax.random.fold_in(jax.random.fold_in(own_key, 6), position), (shards_of,), jnp.float32, smallest / len(cuts), largest / len(cuts))
        loudness = loudness * jnp.repeat(jnp.exp(steps), shape[position] // shards_of).reshape((-1,) + (1,) * (len(shape) - 1 - position))
    return loudness


def bell_draw(key, extent, deviation, most, split=(), kind=jnp.bfloat16):
    loudness = steps_of(key, extent, split, -0.22, 0.18) if split else 1.0
    array = jax.random.normal(key, extent, jnp.float32) * deviation * loudness
    return jnp.minimum(jnp.maximum(array, -most), most).astype(kind)


def setup_inputs(seed: int = 0) -> dict:
    seeds = jax.random.split(jax.random.key(seed), 18)
    return {
        "latent": draw_latent(jax.random.fold_in(seeds[17], 71), 0),
        "cond": bell_draw(seeds[1], (D,), 1.0, 6.0, (), jnp.float32),
        "ctx_mod": bell_draw(seeds[2], (D,), 1.0, 6.0, (), jnp.float32),
        "context": bell_draw(seeds[3], (CTX, D), 1.0, 6.0, ((0, 32),)),
        "shift_w": bell_draw(seeds[4], (D, D), D ** -0.5, 0.125, ((0, 16), (1, 2)), jnp.float32),
        "scale_w": bell_draw(seeds[5], (D, D), D ** -0.5, 0.125, ((0, 16), (1, 2)), jnp.float32),
        "gate_w": bell_draw(seeds[6], (D, D), D ** -0.5, 0.125, ((0, 16), (1, 2)), jnp.float32),
        "norm_gain": jnp.clip(1.0 + 0.18 * jax.random.normal(seeds[7], (D,), jnp.float32), 0.1, 1.9),
        "w_qn": bell_draw(seeds[8], (D, HEADS * NOPE), D ** -0.5, 0.125, ((1, 2),)),
        "w_qr": draw_w_qr(jax.random.fold_in(seeds[17], 71), 0),
        "w_kv_down": bell_draw(seeds[10], (D, KV_RANK), D ** -0.5, 0.125),
        "w_rope_key": draw_w_rope_key(jax.random.fold_in(seeds[17], 71), 0),
        "kv_gain": jnp.clip(1.0 + 0.18 * jax.random.normal(seeds[12], (KV_RANK,), jnp.float32), 0.1, 1.9),
        "w_key_up": bell_draw(seeds[13], (KV_RANK, HEADS * NOPE), (2.5 * KV_RANK ** -0.5), 0.66015625, ((1, 2),)),
        "w_value_up": bell_draw(seeds[14], (KV_RANK, HEADS * VDIM), KV_RANK ** -0.5, 0.25, ((1, 2),)),
        "ctx_bias": jnp.clip(2.0 + 1.5 * jax.random.uniform(seeds[15], (HEADS,), jnp.float32) ** steps_of(seeds[15], (HEADS,), ((0, 2),), -0.2, 0.2), 2.0, 3.5),
        "w_out": bell_draw(seeds[16], (HEADS * VDIM, D), (4.0 * (HEADS * VDIM) ** -0.5), 0.52734375, ((0, 2),)),
    }


EPS = 1e-06
ROPE_BASE = 10000.0

def modulate(rows_in, gain, shift, scale):
    values = rows_in.astype(jnp.float32)
    normed = values * lax.rsqrt(lax.optimization_barrier(jnp.mean(values * values, axis=-1, keepdims=True)) + EPS)
    return (normed * gain * (1.0 + scale) + shift).astype(jnp.bfloat16)

def compress(rows_in, w_kv_down, kv_gain):
    inner = jnp.dot(rows_in, w_kv_down, preferred_element_type=jnp.float32)
    normed = inner * lax.rsqrt(lax.optimization_barrier(jnp.mean(inner * inner, axis=-1, keepdims=True)) + EPS)
    return (normed * kv_gain).astype(jnp.bfloat16)

def angles(positions):
    quarter = ROPE // 4
    inverse = ROPE_BASE ** (-jnp.arange(quarter, dtype=jnp.float32) / quarter)
    row = (positions // GRID_W).astype(jnp.float32)
    column = (positions % GRID_W).astype(jnp.float32)
    return jnp.concatenate([row[:, None] * inverse[None, :], column[:, None] * inverse[None, :]], axis=-1)

def rotate(values, angle):
    pairs = values.reshape(values.shape[:-1] + (values.shape[-1] // 2, 2))
    first = pairs[..., 0]
    second = pairs[..., 1]
    cosine = jnp.cos(angle)
    sine = jnp.sin(angle)
    turned = jnp.stack([first * cosine - second * sine, first * sine + second * cosine], axis=-1)
    return turned.reshape(values.shape)

def reference(latent, cond, ctx_mod, context, shift_w, scale_w, gate_w, norm_gain, w_qn, w_qr, w_kv_down, w_rope_key, kv_gain, w_key_up, w_value_up, ctx_bias, w_out):
    pair = jnp.stack([jax.nn.silu(cond), jax.nn.silu(ctx_mod)])
    shift = jnp.dot(pair, shift_w, precision=lax.Precision.HIGHEST)
    scale = jnp.dot(pair, scale_w, precision=lax.Precision.HIGHEST)
    gate = jnp.dot(pair, gate_w, precision=lax.Precision.HIGHEST)
    h_rows = modulate(latent, norm_gain, shift[0], scale[0])
    h_ctx = modulate(context, norm_gain, shift[1], scale[1])
    turn = angles(jnp.arange(SEQ, dtype=jnp.int32))
    query_nope = jnp.dot(h_rows, w_qn, preferred_element_type=jnp.float32).astype(jnp.bfloat16)
    query_nope = query_nope.reshape(SEQ, HEADS, NOPE)
    query_rope = jnp.dot(h_rows, w_qr, preferred_element_type=jnp.float32).reshape(SEQ, HEADS, ROPE)
    query_rope = rotate(query_rope, turn[:, None, :]).astype(jnp.bfloat16)
    latents = jnp.concatenate([compress(h_rows, w_kv_down, kv_gain), compress(h_ctx, w_kv_down, kv_gain)], axis=0)
    rope_rows = rotate(jnp.dot(h_rows, w_rope_key, preferred_element_type=jnp.float32), turn).astype(jnp.bfloat16)
    rope_ctx = jnp.dot(h_ctx, w_rope_key, preferred_element_type=jnp.float32).astype(jnp.bfloat16)
    rope_keys = jnp.concatenate([rope_rows, rope_ctx], axis=0)
    total_keys = SEQ + CTX
    keys = jnp.dot(latents, w_key_up, preferred_element_type=jnp.float32).astype(jnp.bfloat16)
    keys = keys.reshape(total_keys, HEADS, NOPE).astype(jnp.float32)
    values = jnp.dot(latents, w_value_up, preferred_element_type=jnp.float32).astype(jnp.bfloat16)
    values = values.reshape(total_keys, HEADS, VDIM).astype(jnp.float32)
    rope_wide = rope_keys.astype(jnp.float32)
    is_ctx = jnp.concatenate([jnp.zeros((SEQ,), jnp.float32), jnp.ones((CTX,), jnp.float32)])
    offset = ctx_bias[:, None] * is_ctx[None, :]
    factor = (NOPE + ROPE) ** (-0.5)
    block = 512
    count = SEQ // block

    def attend(pieces):
        nope_block, rope_block = pieces
        scores = jnp.einsum('qhd,khd->hqk', nope_block.astype(jnp.float32), keys)
        scores = scores + jnp.einsum('qhr,kr->hqk', rope_block.astype(jnp.float32), rope_wide)
        scores = scores * factor + offset[:, None, :]
        top = lax.optimization_barrier(jnp.max(scores, axis=-1, keepdims=True))
        weights = jnp.exp(scores - top)
        total = lax.optimization_barrier(jnp.sum(weights, axis=-1))
        rounded = lax.optimization_barrier(weights.astype(jnp.bfloat16))
        mixed_heads = jnp.einsum('hqk,khd->qhd', rounded.astype(jnp.float32), values)
        result = mixed_heads / jnp.transpose(total)[:, :, None]
        return result.reshape(block, HEADS * VDIM).astype(jnp.bfloat16)
    attended = lax.map(attend, (query_nope.reshape(count, block, HEADS, NOPE), query_rope.reshape(count, block, HEADS, ROPE)))
    attended = attended.reshape(SEQ, HEADS * VDIM)
    group = HEADS_DEV * VDIM

    def add_group(index, total):
        part = lax.dynamic_slice_in_dim(attended, index * group, group, 1)
        rows_part = lax.dynamic_slice_in_dim(w_out, index * group, group, 0)
        term = jnp.dot(part, rows_part, preferred_element_type=jnp.float32).astype(jnp.bfloat16)
        term = lax.optimization_barrier(term)
        return total + term.astype(jnp.float32)
    branch = lax.fori_loop(0, N_TP, add_group, jnp.zeros((SEQ, D), jnp.float32))
    return (latent.astype(jnp.float32) + gate[0] * branch).astype(jnp.bfloat16)
```

```python
import functools

import jax
import jax.numpy as jnp
from jax import lax
from jax.experimental import pallas as pl
from jax.experimental.pallas import tpu as pltpu
from jax.sharding import PartitionSpec as P

GRID_W = 128
EPS = 1e-06
ROPE_BASE = 10000.0
LANES = 128
LOG2E = 1.4426950408889634
FLAGS = 4
MESH = pl.DeviceIdType.MESH
F32 = jnp.float32
BF16 = jnp.bfloat16


def remote(src, dst, send, recv, device):
    return pltpu.make_async_remote_copy(
        src_ref=src, dst_ref=dst, send_sem=send, recv_sem=recv, device_id=device, device_id_type=MESH
    )


def rotate(values, cosine, sine):
    width = values.shape[-1]
    ahead = pltpu.roll(values, width - 1, 1)
    behind = pltpu.roll(values, 1, 1)
    even = lax.broadcasted_iota(jnp.int32, values.shape, 1) % 2 == 0
    return values * cosine + jnp.where(even, ahead, behind) * sine


def modulation_kernel(
    n_sp, n_tp, rows, ctx_rows,
    pair_ref, shift_w, scale_w, gate_w, x_ref, gain_ref, down_ref, rope_ref, kv_gain_ref, cos_ref, sin_ref,
    h_ref, packed_ref, gate_ref,
    part, landed, reduced, full, mods, send1, recv1, send2, recv2,
):
    me = lax.axis_index("sp")
    mine = lax.axis_index("tp")
    total = n_sp * n_tp
    flat = me * n_tp + mine
    barrier = pltpu.get_barrier_semaphore()

    def greet(i, _):
        other = lax.rem(flat + i, total)
        pl.semaphore_signal(barrier, inc=1, device_id=(other // n_tp, other % n_tp), device_id_type=MESH)
        return 0

    lax.fori_loop(1, total, greet, 0)

    columns = shift_w.shape[1]
    blocks = columns // LANES
    per = -(-6 * blocks // n_sp)
    part[...] = jnp.zeros_like(part)
    pair = pair_ref[...]
    for which, weight in enumerate((shift_w, scale_w, gate_w)):
        product = jnp.dot(pair, weight[...], precision=lax.Precision.HIGHEST, preferred_element_type=F32)
        for row in range(2):
            for block in range(blocks):
                unit = (which * 2 + row) * blocks + block
                part[unit // per, unit % per : unit % per + 1, :] = product[
                    row : row + 1, block * LANES : (block + 1) * LANES
                ]
    pl.semaphore_wait(barrier, total - 1)

    def scatter(i, _):
        other = lax.rem(me + i, n_sp)
        remote(part.at[other], landed.at[me], send1.at[other], recv1.at[me], (other, mine)).start()
        return 0

    lax.fori_loop(1, n_sp, scatter, 0)
    landed[me] = part[me]

    def scattered(i, _):
        other = lax.rem(me + i, n_sp)
        remote(part.at[other], landed.at[other], send1.at[other], recv1.at[other], (other, mine)).wait()
        return 0

    lax.fori_loop(1, n_sp, scattered, 0)
    reduced[...] = jnp.sum(landed[...], axis=0)

    def gather(i, _):
        other = lax.rem(flat + i, total)
        remote(
            reduced, full.at[flat], send2.at[other], recv2.at[flat], (other // n_tp, other % n_tp)
        ).start()
        return 0

    lax.fori_loop(1, total, gather, 0)
    full[flat] = reduced[...]
    x = x_ref[...].astype(F32)
    normed = x * lax.rsqrt(jnp.mean(x * x, axis=-1, keepdims=True) + EPS) * gain_ref[...]

    def gathered(i, _):
        other = lax.rem(flat + i, total)
        remote(
            reduced, full.at[other], send2.at[other], recv2.at[other], (other // n_tp, other % n_tp)
        ).wait()
        return 0

    lax.fori_loop(1, total, gathered, 0)
    for unit in range(6 * blocks):
        row, block = unit // blocks, unit % blocks
        for t in range(n_tp):
            at = t * columns + block * LANES
            mods[row : row + 1, at : at + LANES] = full[(unit // per) * n_tp + t, unit % per : unit % per + 1, :]
    index = lax.broadcasted_iota(jnp.int32, (x.shape[0], 1), 0)
    latent_row = index < rows
    shift = jnp.where(latent_row, mods[0:1, :], mods[1:2, :])
    scale = jnp.where(latent_row, mods[2:3, :], mods[3:4, :])
    h = (normed * (1.0 + scale) + shift).astype(BF16)
    gate_ref[...] = mods[4:5, :]
    h_ref[...] = h[:rows]
    inner = jnp.dot(h, down_ref[...], preferred_element_type=F32)
    inner = inner * lax.rsqrt(jnp.mean(inner * inner, axis=-1, keepdims=True) + EPS)
    rank = inner.shape[1]
    packed_ref[:, :rank] = (inner * kv_gain_ref[...]).astype(BF16)
    rope = rope_ref.shape[1]
    key = jnp.dot(h, rope_ref[...], preferred_element_type=F32)
    key = jnp.concatenate([key, jnp.zeros((key.shape[0], LANES - rope), F32)], axis=1)
    key = rotate(key, cos_ref[...], sin_ref[...])
    lane = lax.broadcasted_iota(jnp.int32, key.shape, 1)
    is_ctx = (index >= rows) & (index < rows + ctx_rows)
    is_pad = index >= rows + ctx_rows
    flag = jnp.where(lane < rope + FLAGS - 1, is_ctx.astype(F32), is_pad.astype(F32))
    key = jnp.where(lane < rope, key, jnp.where(lane < rope + FLAGS, flag, 0.0))
    packed_ref[:, rank:] = key.astype(BF16)


def attention_kernel(
    n_sp, n_tp, heads, nope, rope, factor,
    h_ref, packed_ref, bias_ref, cos_ref, sin_ref, qn_ref, qr_ref, ku_ref, vu_ref, wo_ref, latent_ref, gate_ref,
    out_ref,
    buf, hbuf, q, acc, top, total, att, outbox, inbox, send, recv, send_t, recv_t, send_h, recv_h, send_o, recv_o,
):
    me = lax.axis_index("sp")
    mine = lax.axis_index("tp")
    nz = n_sp // 4
    z, side = me // 4, me % 4
    y, x = side // 2, side % 2
    odd = mine % 2
    flip_x = y * 2 + (1 - x)
    flip_y = (1 - y) * 2 + x
    side_a = flip_x * (1 - odd) + flip_y * odd
    side_b = flip_y * (1 - odd) + flip_x * odd
    side_ab = 3 - side
    rows = h_ref.shape[0]
    period, width = packed_ref.shape
    rank = ku_ref.shape[0]

    def column_of(step, t):
        return lax.rem(z + step * (1 - 2 * (t % 2)) + 2 * nz, nz)

    def column(step):
        return column_of(step, mine)

    def peer(zz, ss):
        return (zz * 4 + ss, mine)

    ahead, back = peer(column(1), side), peer(column(-1), side)
    to_a, to_b = peer(z, side_a), peer(z, side_b)
    partners = [lax.rem(mine + i, n_tp) for i in range(1, n_tp)]

    barrier = pltpu.get_barrier_semaphore()
    for other in [ahead, back, to_a, to_b] + [(me, t) for t in partners]:
        pl.semaphore_signal(barrier, inc=1, device_id=other, device_id_type=MESH)
    pl.semaphore_wait(barrier, 3 + n_tp)

    def slot(zz, ss, t):
        return buf.at[t, zz, pl.ds(pl.multiple_of(ss * period, period), period)]

    started = []

    def push(zz, ss, way, device):
        src = packed_ref if way[1] else slot(zz, ss, mine)
        copy = remote(src, slot(zz, ss, mine), send.at[way[0], zz, ss], recv.at[zz, ss], device)
        copy.start()
        started.append(copy)

    def across(zz, ss, own=False):
        src = packed_ref if own else slot(zz, ss, mine)
        for t in partners:
            copy = remote(src, slot(zz, ss, mine), send_t.at[t, zz, ss], recv_t.at[mine, zz, ss], (me, t))
            copy.start()
            started.append(copy)

    def arrived(zz, ss):
        remote(slot(zz, ss, mine), slot(zz, ss, mine), send.at[0, zz, ss], recv.at[zz, ss], ahead).wait_recv()

    forward = nz // 2
    backward = nz - 1 - forward
    order = [0]
    for j in range(1, forward + 1):
        order.append(-j)
        if j <= backward:
            order.append(j)

    for t in partners:
        copy = remote(h_ref, hbuf.at[mine], send_h.at[t], recv_h.at[mine], (me, t))
        copy.start()
        started.append(copy)

    def event_z(step):
        zz = column(step)
        own = step == 0
        if not own:
            arrived(zz, side)
        if own or (step < 0 and -step < forward):
            push(zz, side, (0, own), ahead)
        if own or (step > 0 and step < backward):
            push(zz, side, (1, own), back)
        push(zz, side, (2, own), to_a)
        push(zz, side, (3, own), to_b)
        across(zz, side, own)

    def event_a(step):
        zz = column(step)
        arrived(zz, side_a)
        push(zz, side_a, (3, False), to_b)
        across(zz, side_a)

    def event_b(step, which):
        zz = column(step)
        arrived(zz, which)
        across(zz, which)

    def ready(step):
        for t in partners:
            zz = column_of(step, t)
            for ss in (side, side_a, side_b, side_ab):
                remote(slot(zz, ss, t), slot(zz, ss, t), send_t.at[t, zz, ss], recv_t.at[t, zz, ss], (me, t)).wait_recv()

    event_z(0)
    hbuf[mine] = h_ref[...]
    buf[mine, z, pl.ds(pl.multiple_of(side * period, period), period), :] = packed_ref[...]
    acc[...] = jnp.zeros_like(acc)
    top[...] = jnp.full(top.shape, -1e38, F32)
    total[...] = jnp.zeros_like(total)
    for t in partners:
        remote(h_ref, hbuf.at[t], send_h.at[t], recv_h.at[t], (me, t)).wait_recv()

    tokens = n_tp * rows
    piece = hbuf[...].reshape(tokens, hbuf.shape[2])
    turned = jnp.dot(piece, qr_ref[...], preferred_element_type=F32)
    copies = turned.shape[1] // LANES
    turned = rotate(
        turned, jnp.concatenate([cos_ref[...]] * copies, axis=1), jnp.concatenate([sin_ref[...]] * copies, axis=1)
    ).astype(BF16)
    for head in range(heads):
        q[head, :, :nope] = jnp.dot(
            piece, qn_ref[:, head * nope : (head + 1) * nope], preferred_element_type=F32
        ).astype(BF16)
        q[head, :, nope : nope + rope] = turned[:, head * rope : (head + 1) * rope]
        q[head, :, nope + rope :] = jnp.broadcast_to(
            bias_ref[head : head + 1, :], (tokens, LANES - rope)
        )

    def attend(step):
        places = [(t, column_of(step, t)) for t in range(n_tp)]

        def one(head, _):
            at = pl.ds(pl.multiple_of(head * nope, nope), nope)
            weight = jnp.concatenate([ku_ref[:, at], vu_ref[:, at]], axis=1)
            latents = jnp.concatenate([buf[t, zz, :, :rank] for t, zz in places], axis=0)
            extra = jnp.concatenate([buf[t, zz, :, rank:] for t, zz in places], axis=0)
            both = jnp.dot(latents, weight, preferred_element_type=F32).astype(BF16)
            keys = jnp.concatenate([both[:, :nope], extra], axis=1)
            scores = lax.dot_general(q[head], keys, (((1,), (1,)), ((), ())), preferred_element_type=F32)
            old = top[head][:, :1]
            new = jnp.maximum(old, jnp.max(scores, axis=-1, keepdims=True))
            weights = jnp.exp2((scores - new) * (factor * LOG2E))
            fade = jnp.exp2((old - new) * (factor * LOG2E))
            top[head] = jnp.broadcast_to(new, top.shape[1:])
            total[head] = total[head] * fade + jnp.sum(weights, axis=-1, keepdims=True)
            acc[head] = acc[head] * fade + jnp.dot(
                weights.astype(BF16), both[:, nope:], preferred_element_type=F32
            )
            return 0

        lax.fori_loop(0, heads, one, 0, unroll=min(2, heads))

    def events(step):
        event_z(step)
        event_a(step)
        event_b(step, side_b)
        event_b(step, side_ab)

    event_a(0)
    event_b(0, side_b)
    event_b(0, side_ab)
    ready(0)
    for i, step in enumerate(order):
        if i + 1 < len(order):
            event_z(order[i + 1])
        attend(step)
        if i + 1 < len(order):
            event_a(order[i + 1])
            event_b(order[i + 1], side_b)
            event_b(order[i + 1], side_ab)
            ready(order[i + 1])

    for head in range(heads):
        att[:, head * nope : (head + 1) * nope] = (acc[head] / total[head]).astype(BF16)

    for t in partners:
        lines = pl.ds(pl.multiple_of(t * rows, rows), rows)
        outbox[t] = jnp.dot(att[lines, :], wo_ref[...], preferred_element_type=F32).astype(BF16)
        copy = remote(outbox.at[t], inbox.at[mine], send_o.at[t], recv_o.at[mine], (me, t))
        copy.start()
        started.append(copy)
    lines = pl.ds(pl.multiple_of(mine * rows, rows), rows)
    branch = jnp.dot(att[lines, :], wo_ref[...], preferred_element_type=F32).astype(BF16).astype(F32)
    for t in partners:
        remote(outbox.at[t], inbox.at[t], send_o.at[t], recv_o.at[t], (me, t)).wait_recv()
        branch = branch + inbox[t].astype(F32)
    out_ref[...] = (latent_ref[...].astype(F32) + gate_ref[...] * branch).astype(BF16)
    for copy in started:
        copy.wait_send()


def tables(positions, rope, real):
    quarter = rope // 4
    lane = jnp.arange(LANES, dtype=jnp.int32)
    pair = (lane % rope) // 2
    inverse = ROPE_BASE ** (-(pair % quarter).astype(F32) / quarter)
    place = jnp.where(pair[None, :] < quarter, (positions // GRID_W)[:, None], (positions % GRID_W)[:, None])
    angle = jnp.where(real[:, None], place.astype(F32) * inverse[None, :], 0.0)
    sine = jnp.sin(angle)
    return jnp.cos(angle), jnp.where(lane[None, :] % 2 == 0, -sine, sine)


def body(
    latent, cond, ctx_mod, context, shift_w, scale_w, gate_w, norm_gain, w_qn, w_qr, w_kv_down, w_rope_key,
    kv_gain, w_key_up, w_value_up, ctx_bias, w_out,
):
    n_sp, n_tp = lax.axis_size("sp"), lax.axis_size("tp")
    sp_index, tp_index = lax.axis_index("sp"), lax.axis_index("tp")
    rows, width = latent.shape
    ctx_rows = context.shape[0]
    tokens = rows * n_tp
    heads = ctx_bias.shape[0]
    nope = w_key_up.shape[1] // heads
    rope = w_rope_key.shape[1]
    rank = w_kv_down.shape[1]
    period = -(-(rows + ctx_rows) // 16) * 16
    factor = (nope + rope) ** (-0.5)
    feat = shift_w.shape[0]
    pair = jnp.stack([jax.nn.silu(cond), jax.nn.silu(ctx_mod)])
    pair = lax.dynamic_slice_in_dim(pair, sp_index * feat, feat, 1)
    pair = jnp.concatenate([pair, jnp.zeros((6, feat), F32)], axis=0)
    pad = jnp.zeros((period - rows - ctx_rows, width), BF16)
    x = jnp.concatenate([latent, context, pad], axis=0)
    line = jnp.arange(period, dtype=jnp.int32)
    own_cos, own_sin = tables(sp_index * tokens + tp_index * rows + line, rope, line < rows)
    place = jnp.arange(tokens, dtype=jnp.int32)
    cosine, sine = tables(sp_index * tokens + place, rope, place >= 0)

    vmem = pl.BlockSpec(memory_space=pltpu.VMEM)
    dma = pltpu.SemaphoreType.DMA
    h, packed, gate = pl.pallas_call(
        functools.partial(modulation_kernel, n_sp, n_tp, rows, ctx_rows),
        out_shape=(
            jax.ShapeDtypeStruct((rows, width), BF16),
            jax.ShapeDtypeStruct((period, rank + LANES), BF16),
            jax.ShapeDtypeStruct((1, width), F32),
        ),
        in_specs=[vmem] * 11,
        out_specs=(vmem,) * 3,
        scratch_shapes=[
            pltpu.VMEM((n_sp, 8, LANES), F32),
            pltpu.VMEM((n_sp, 8, LANES), F32),
            pltpu.VMEM((8, LANES), F32),
            pltpu.VMEM((n_sp * n_tp, 8, LANES), F32),
            pltpu.VMEM((8, width), F32),
            dma((n_sp,)),
            dma((n_sp,)),
            dma((n_sp * n_tp,)),
            dma((n_sp * n_tp,)),
        ],
        compiler_params=pltpu.CompilerParams(
            collective_id=0, has_side_effects=True, vmem_limit_bytes=40 * 1024 * 1024
        ),
        name="modulation",
    )(
        pair, shift_w, scale_w, gate_w, x, norm_gain[None, :], w_kv_down, w_rope_key, kv_gain[None, :],
        own_cos, own_sin,
    )

    scaled = ctx_bias / factor
    high = lax.reduce_precision(scaled, 8, 7)
    middle = lax.reduce_precision(scaled - high, 8, 7)
    low = scaled - high - middle
    bias = jnp.stack([high, middle, low, jnp.full_like(scaled, -1e30)], axis=1)
    bias = jnp.concatenate([bias, jnp.zeros((heads, LANES - rope - FLAGS), F32)], axis=1).astype(BF16)
    short = -(heads * rope) % LANES
    if short:
        w_qr = jnp.concatenate([w_qr, jnp.zeros((width, short), BF16)], axis=1)

    nz = n_sp // 4
    return pl.pallas_call(
        functools.partial(attention_kernel, n_sp, n_tp, heads, nope, rope, factor),
        out_shape=jax.ShapeDtypeStruct((rows, width), BF16),
        in_specs=[vmem] * 12,
        out_specs=vmem,
        scratch_shapes=[
            pltpu.VMEM((n_tp, nz, 4 * period, rank + LANES), BF16),
            pltpu.VMEM((n_tp, rows, width), BF16),
            pltpu.VMEM((heads, tokens, nope + LANES), BF16),
            pltpu.VMEM((heads, tokens, nope), F32),
            pltpu.VMEM((heads, tokens, LANES), F32),
            pltpu.VMEM((heads, tokens, LANES), F32),
            pltpu.VMEM((tokens, heads * nope), BF16),
            pltpu.VMEM((n_tp, rows, width), BF16),
            pltpu.VMEM((n_tp, rows, width), BF16),
            dma((4, nz, 4)),
            dma((nz, 4)),
            dma((n_tp, nz, 4)),
            dma((n_tp, nz, 4)),
            dma((n_tp,)),
            dma((n_tp,)),
            dma((n_tp,)),
            dma((n_tp,)),
        ],
        compiler_params=pltpu.CompilerParams(
            collective_id=1, has_side_effects=True, vmem_limit_bytes=60 * 1024 * 1024
        ),
        name="attention",
    )(h, packed, bias, cosine, sine, w_qn, w_qr, w_key_up, w_value_up, w_out, latent, gate)


def solution(mesh):
    placed = (
        P(("sp", "tp"), None),
        P(),
        P(),
        P(("sp", "tp"), None),
        P("sp", "tp"),
        P("sp", "tp"),
        P("sp", "tp"),
        P(),
        P(None, "tp"),
        P(None, "tp"),
        P(),
        P(),
        P(),
        P(None, "tp"),
        P(None, "tp"),
        P("tp"),
        P("tp", None),
    )
    return jax.shard_map(
        body, mesh=mesh, in_specs=placed, out_specs=P(("sp", "tp"), None), check_vma=False
    )
```

```python
import functools

import jax
import jax.numpy as jnp
from jax import lax
from jax.experimental import pallas as pl
from jax.experimental.pallas import tpu as pltpu
from jax.sharding import PartitionSpec as P

GRID_W = 128
EPS = 1e-06
ROPE_BASE = 10000.0
LANES = 128
LOG2E = 1.4426950408889634
FLAGS = 4
MESH = pl.DeviceIdType.MESH
F32 = jnp.float32
BF16 = jnp.bfloat16


def remote(src, dst, send, recv, device):
    return pltpu.make_async_remote_copy(
        src_ref=src, dst_ref=dst, send_sem=send, recv_sem=recv, device_id=device, device_id_type=MESH
    )


def rotate(values, cosine, sine):
    width = values.shape[-1]
    ahead = pltpu.roll(values, width - 1, 1)
    behind = pltpu.roll(values, 1, 1)
    even = lax.broadcasted_iota(jnp.int32, values.shape, 1) % 2 == 0
    return values * cosine + jnp.where(even, ahead, behind) * sine


def modulation_kernel(
    n_sp, n_tp, rows, ctx_rows,
    pair_ref, shift_w, scale_w, gate_w, x_ref, gain_ref, down_ref, rope_ref, kv_gain_ref, cos_ref, sin_ref,
    h_ref, packed_ref, gate_ref,
    part, landed, reduced, full, mods, send1, recv1, send2, recv2,
):
    me = lax.axis_index("sp")
    mine = lax.axis_index("tp")
    total = n_sp * n_tp
    flat = me * n_tp + mine
    barrier = pltpu.get_barrier_semaphore()

    def greet(i, _):
        other = lax.rem(flat + i, total)
        pl.semaphore_signal(barrier, inc=1, device_id=(other // n_tp, other % n_tp), device_id_type=MESH)
        return 0

    lax.fori_loop(1, total, greet, 0)

    columns = shift_w.shape[1]
    blocks = columns // LANES
    per = -(-6 * blocks // n_sp)
    part[...] = jnp.zeros_like(part)
    pair = pair_ref[...]
    for which, weight in enumerate((shift_w, scale_w, gate_w)):
        product = jnp.dot(pair, weight[...], precision=lax.Precision.HIGHEST, preferred_element_type=F32)
        for row in range(2):
            for block in range(blocks):
                unit = (which * 2 + row) * blocks + block
                part[unit // per, unit % per : unit % per + 1, :] = product[
                    row : row + 1, block * LANES : (block + 1) * LANES
                ]
    pl.semaphore_wait(barrier, total - 1)

    def scatter(i, _):
        other = lax.rem(me + i, n_sp)
        remote(part.at[other], landed.at[me], send1.at[other], recv1.at[me], (other, mine)).start()
        return 0

    lax.fori_loop(1, n_sp, scatter, 0)
    landed[me] = part[me]

    def scattered(i, _):
        other = lax.rem(me + i, n_sp)
        remote(part.at[other], landed.at[other], send1.at[other], recv1.at[other], (other, mine)).wait()
        return 0

    lax.fori_loop(1, n_sp, scattered, 0)
    reduced[...] = jnp.sum(landed[...], axis=0)

    def gather(i, _):
        other = lax.rem(flat + i, total)
        remote(
            reduced, full.at[flat], send2.at[other], recv2.at[flat], (other // n_tp, other % n_tp)
        ).start()
        return 0

    lax.fori_loop(1, total, gather, 0)
    full[flat] = reduced[...]
    x = x_ref[...].astype(F32)
    normed = x * lax.rsqrt(jnp.mean(x * x, axis=-1, keepdims=True) + EPS) * gain_ref[...]

    def gathered(i, _):
        other = lax.rem(flat + i, total)
        remote(
            reduced, full.at[other], send2.at[other], recv2.at[other], (other // n_tp, other % n_tp)
        ).wait()
        return 0

    lax.fori_loop(1, total, gathered, 0)
    for unit in range(6 * blocks):
        row, block = unit // blocks, unit % blocks
        for t in range(n_tp):
            at = t * columns + block * LANES
            mods[row : row + 1, at : at + LANES] = full[(unit // per) * n_tp + t, unit % per : unit % per + 1, :]
    index = lax.broadcasted_iota(jnp.int32, (x.shape[0], 1), 0)
    latent_row = index < rows
    shift = jnp.where(latent_row, mods[0:1, :], mods[1:2, :])
    scale = jnp.where(latent_row, mods[2:3, :], mods[3:4, :])
    h = (normed * (1.0 + scale) + shift).astype(BF16)
    gate_ref[...] = mods[4:5, :]
    h_ref[...] = h[:rows]
    inner = jnp.dot(h, down_ref[...], preferred_element_type=F32)
    inner = inner * lax.rsqrt(jnp.mean(inner * inner, axis=-1, keepdims=True) + EPS)
    rank = inner.shape[1]
    packed_ref[:, :rank] = (inner * kv_gain_ref[...]).astype(BF16)
    rope = rope_ref.shape[1]
    key = jnp.dot(h, rope_ref[...], preferred_element_type=F32)
    key = jnp.concatenate([key, jnp.zeros((key.shape[0], LANES - rope), F32)], axis=1)
    key = rotate(key, cos_ref[...], sin_ref[...])
    lane = lax.broadcasted_iota(jnp.int32, key.shape, 1)
    is_ctx = (index >= rows) & (index < rows + ctx_rows)
    is_pad = index >= rows + ctx_rows
    flag = jnp.where(lane < rope + FLAGS - 1, is_ctx.astype(F32), is_pad.astype(F32))
    key = jnp.where(lane < rope, key, jnp.where(lane < rope + FLAGS, flag, 0.0))
    packed_ref[:, rank:] = key.astype(BF16)


def attention_kernel(
    n_sp, n_tp, heads, nope, rope, factor,
    h_ref, packed_ref, bias_ref, cos_ref, sin_ref, qn_hbm, qr_hbm, ku_hbm, vu_hbm, wo_hbm, latent_ref, gate_ref,
    out_ref,
    qr_ref, qn_ref, ku_ref, vu_ref, wo_ref, load_sem,
    buf, hbuf, q, acc, top, total, att, outbox, inbox, send, recv, send_t, recv_t, send_h, recv_h, send_o, recv_o,
):
    me = lax.axis_index("sp")
    mine = lax.axis_index("tp")
    loads = [
        pltpu.make_async_copy(src, dst, load_sem.at[i])
        for i, (src, dst) in enumerate(
            ((qr_hbm, qr_ref), (qn_hbm, qn_ref), (ku_hbm, ku_ref), (vu_hbm, vu_ref), (wo_hbm, wo_ref))
        )
    ]
    for load in loads:
        load.start()
    nz = n_sp // 4
    z, side = me // 4, me % 4
    y, x = side // 2, side % 2
    odd = mine % 2
    flip_x = y * 2 + (1 - x)
    flip_y = (1 - y) * 2 + x
    side_a = flip_x * (1 - odd) + flip_y * odd
    side_b = flip_y * (1 - odd) + flip_x * odd
    side_ab = 3 - side
    rows = h_ref.shape[0]
    period, width = packed_ref.shape
    rank = ku_ref.shape[0]

    def column_of(step, t):
        return lax.rem(z + step * (1 - 2 * (t % 2)) + 2 * nz, nz)

    def column(step):
        return column_of(step, mine)

    def peer(zz, ss):
        return (zz * 4 + ss, mine)

    ahead, back = peer(column(1), side), peer(column(-1), side)
    to_a, to_b = peer(z, side_a), peer(z, side_b)
    partners = [lax.rem(mine + i, n_tp) for i in range(1, n_tp)]

    barrier = pltpu.get_barrier_semaphore()
    for other in [ahead, back, to_a, to_b] + [(me, t) for t in partners]:
        pl.semaphore_signal(barrier, inc=1, device_id=other, device_id_type=MESH)
    pl.semaphore_wait(barrier, 3 + n_tp)

    def slot(zz, ss, t):
        return buf.at[t, zz, pl.ds(pl.multiple_of(ss * period, period), period)]

    started = []

    def link(step, ss, way, own, device):
        zz = column(step)
        src = packed_ref if own else slot(zz, ss, mine)
        return remote(src, slot(zz, ss, mine), send.at[way, zz, ss], recv.at[zz, ss], device)

    def over(step, ss, own, t):
        zz = column(step)
        src = packed_ref if own else slot(zz, ss, mine)
        return remote(src, slot(zz, ss, mine), send_t.at[t, zz, ss], recv_t.at[mine, zz, ss], (me, t))

    def push(step, ss, way, own, device):
        link(step, ss, way, own, device).start()
        started.append(lambda: link(step, ss, way, own, device))

    def across(step, ss, own=False):
        for t in partners:
            over(step, ss, own, t).start()
            started.append(lambda t=t: over(step, ss, own, t))

    def arrived(zz, ss):
        remote(slot(zz, ss, mine), slot(zz, ss, mine), send.at[0, zz, ss], recv.at[zz, ss], ahead).wait_recv()

    forward = nz // 2
    backward = nz - 1 - forward
    order = [0]
    for j in range(1, forward + 1):
        order.append(-j)
        if j <= backward:
            order.append(j)

    for t in partners:
        copy = remote(h_ref, hbuf.at[mine], send_h.at[t], recv_h.at[mine], (me, t))
        copy.start()
        started.append(lambda copy=copy: copy)

    def event_z(step):
        zz = column(step)
        own = step == 0
        if not own:
            arrived(zz, side)
        if own or (step < 0 and -step < forward):
            push(step, side, 0, own, ahead)
        if own or (step > 0 and step < backward):
            push(step, side, 1, own, back)
        push(step, side, 2, own, to_a)
        push(step, side, 3, own, to_b)
        across(step, side, own)

    def event_a(step):
        zz = column(step)
        arrived(zz, side_a)
        push(step, side_a, 3, False, to_b)
        across(step, side_a)

    def event_b(step, which):
        zz = column(step)
        arrived(zz, which)
        across(step, which)

    def ready(step):
        for t in partners:
            zz = column_of(step, t)
            for ss in (side, side_a, side_b, side_ab):
                remote(slot(zz, ss, t), slot(zz, ss, t), send_t.at[t, zz, ss], recv_t.at[t, zz, ss], (me, t)).wait_recv()

    event_z(0)
    hbuf[mine] = h_ref[...]
    buf[mine, z, pl.ds(pl.multiple_of(side * period, period), period), :] = packed_ref[...]
    acc[...] = jnp.zeros_like(acc)
    top[...] = jnp.full(top.shape, -1e38, F32)
    total[...] = jnp.zeros_like(total)
    for t in partners:
        remote(h_ref, hbuf.at[t], send_h.at[t], recv_h.at[t], (me, t)).wait_recv()

    tokens = n_tp * rows
    piece = hbuf[...].reshape(tokens, hbuf.shape[2])
    loads[0].wait()
    turned = jnp.dot(piece, qr_ref[...], preferred_element_type=F32)
    copies = turned.shape[1] // LANES
    turned = rotate(
        turned, jnp.concatenate([cos_ref[...]] * copies, axis=1), jnp.concatenate([sin_ref[...]] * copies, axis=1)
    ).astype(BF16)
    loads[1].wait()
    for head in range(heads):
        q[head, :, :nope] = jnp.dot(
            piece, qn_ref[:, head * nope : (head + 1) * nope], preferred_element_type=F32
        ).astype(BF16)
        q[head, :, nope : nope + rope] = turned[:, head * rope : (head + 1) * rope]
        q[head, :, nope + rope :] = jnp.broadcast_to(
            bias_ref[head : head + 1, :], (tokens, LANES - rope)
        )

    def attend(step, beside):
        places = [(t, column_of(step, t)) for t in range(n_tp)]

        def one(head, _):
            at = pl.ds(pl.multiple_of(head * nope, nope), nope)
            weight = jnp.concatenate([ku_ref[:, at], vu_ref[:, at]], axis=1)
            latents = jnp.concatenate([buf[t, zz, :, :rank] for t, zz in places], axis=0)
            extra = jnp.concatenate([buf[t, zz, :, rank:] for t, zz in places], axis=0)
            both = jnp.dot(latents, weight, preferred_element_type=F32).astype(BF16)
            keys = jnp.concatenate([both[:, :nope], extra], axis=1)
            scores = lax.dot_general(q[head], keys, (((1,), (1,)), ((), ())), preferred_element_type=F32)
            old = top[head][:, :1]
            new = jnp.maximum(old, jnp.max(scores, axis=-1, keepdims=True))
            weights = jnp.exp2((scores - new) * (factor * LOG2E))
            fade = jnp.exp2((old - new) * (factor * LOG2E))
            top[head] = jnp.broadcast_to(new, top.shape[1:])
            total[head] = total[head] * fade + jnp.sum(weights, axis=-1, keepdims=True)
            acc[head] = acc[head] * fade + jnp.dot(
                weights.astype(BF16), both[:, nope:], preferred_element_type=F32
            )
            return 0

        together = 2 if heads % 2 == 0 else 1

        def some(i, _):
            for k, event in enumerate(beside):
                if k < heads // together:
                    pl.when(i == k)(event)
            for j in range(together):
                one(i * together + j, 0)
            return 0

        lax.fori_loop(0, heads // together, some, 0)
        for event in beside[heads // together :]:
            event()

    event_a(0)
    event_b(0, side_b)
    event_b(0, side_ab)
    ready(0)
    loads[2].wait()
    loads[3].wait()
    for i, step in enumerate(order):
        if i + 1 < len(order):
            later = order[i + 1]
            attend(
                step,
                [
                    functools.partial(event_z, later),
                    functools.partial(event_a, later),
                    functools.partial(event_b, later, side_b),
                    functools.partial(event_b, later, side_ab),
                ],
            )
            ready(later)
        else:
            attend(step, [])
    loads[4].wait()

    for head in range(heads):
        att[:, head * nope : (head + 1) * nope] = (acc[head] / total[head]).astype(BF16)

    for t in partners:
        lines = pl.ds(pl.multiple_of(t * rows, rows), rows)
        outbox[t] = jnp.dot(att[lines, :], wo_ref[...], preferred_element_type=F32).astype(BF16)
        copy = remote(outbox.at[t], inbox.at[mine], send_o.at[t], recv_o.at[mine], (me, t))
        copy.start()
        started.append(lambda copy=copy: copy)
    lines = pl.ds(pl.multiple_of(mine * rows, rows), rows)
    branch = jnp.dot(att[lines, :], wo_ref[...], preferred_element_type=F32).astype(BF16).astype(F32)
    for t in partners:
        remote(outbox.at[t], inbox.at[t], send_o.at[t], recv_o.at[t], (me, t)).wait_recv()
        branch = branch + inbox[t].astype(F32)
    out_ref[...] = (latent_ref[...].astype(F32) + gate_ref[...] * branch).astype(BF16)
    for make in started:
        make().wait_send()


def tables(positions, rope, real):
    quarter = rope // 4
    lane = jnp.arange(LANES, dtype=jnp.int32)
    pair = (lane % rope) // 2
    inverse = ROPE_BASE ** (-(pair % quarter).astype(F32) / quarter)
    place = jnp.where(pair[None, :] < quarter, (positions // GRID_W)[:, None], (positions % GRID_W)[:, None])
    angle = jnp.where(real[:, None], place.astype(F32) * inverse[None, :], 0.0)
    sine = jnp.sin(angle)
    return jnp.cos(angle), jnp.where(lane[None, :] % 2 == 0, -sine, sine)


def body(
    latent, cond, ctx_mod, context, shift_w, scale_w, gate_w, norm_gain, w_qn, w_qr, w_kv_down, w_rope_key,
    kv_gain, w_key_up, w_value_up, ctx_bias, w_out,
):
    n_sp, n_tp = lax.axis_size("sp"), lax.axis_size("tp")
    sp_index, tp_index = lax.axis_index("sp"), lax.axis_index("tp")
    rows, width = latent.shape
    ctx_rows = context.shape[0]
    tokens = rows * n_tp
    heads = ctx_bias.shape[0]
    nope = w_key_up.shape[1] // heads
    rope = w_rope_key.shape[1]
    rank = w_kv_down.shape[1]
    period = -(-(rows + ctx_rows) // 16) * 16
    factor = (nope + rope) ** (-0.5)
    feat = shift_w.shape[0]
    pair = jnp.stack([jax.nn.silu(cond), jax.nn.silu(ctx_mod)])
    pair = lax.dynamic_slice_in_dim(pair, sp_index * feat, feat, 1)
    pair = jnp.concatenate([pair, jnp.zeros((6, feat), F32)], axis=0)
    pad = jnp.zeros((period - rows - ctx_rows, width), BF16)
    x = jnp.concatenate([latent, context, pad], axis=0)
    line = jnp.arange(period, dtype=jnp.int32)
    own_cos, own_sin = tables(sp_index * tokens + tp_index * rows + line, rope, line < rows)
    place = jnp.arange(tokens, dtype=jnp.int32)
    cosine, sine = tables(sp_index * tokens + place, rope, place >= 0)

    vmem = pl.BlockSpec(memory_space=pltpu.VMEM)
    dma = pltpu.SemaphoreType.DMA
    h, packed, gate = pl.pallas_call(
        functools.partial(modulation_kernel, n_sp, n_tp, rows, ctx_rows),
        out_shape=(
            jax.ShapeDtypeStruct((rows, width), BF16),
            jax.ShapeDtypeStruct((period, rank + LANES), BF16),
            jax.ShapeDtypeStruct((1, width), F32),
        ),
        in_specs=[vmem] * 11,
        out_specs=(vmem,) * 3,
        scratch_shapes=[
            pltpu.VMEM((n_sp, 8, LANES), F32),
            pltpu.VMEM((n_sp, 8, LANES), F32),
            pltpu.VMEM((8, LANES), F32),
            pltpu.VMEM((n_sp * n_tp, 8, LANES), F32),
            pltpu.VMEM((8, width), F32),
            dma((n_sp,)),
            dma((n_sp,)),
            dma((n_sp * n_tp,)),
            dma((n_sp * n_tp,)),
        ],
        compiler_params=pltpu.CompilerParams(
            collective_id=0, has_side_effects=True, vmem_limit_bytes=40 * 1024 * 1024
        ),
        name="modulation",
    )(
        pair, shift_w, scale_w, gate_w, x, norm_gain[None, :], w_kv_down, w_rope_key, kv_gain[None, :],
        own_cos, own_sin,
    )

    scaled = ctx_bias / factor
    high = lax.reduce_precision(scaled, 8, 7)
    middle = lax.reduce_precision(scaled - high, 8, 7)
    low = scaled - high - middle
    bias = jnp.stack([high, middle, low, jnp.full_like(scaled, -1e30)], axis=1)
    bias = jnp.concatenate([bias, jnp.zeros((heads, LANES - rope - FLAGS), F32)], axis=1).astype(BF16)
    short = -(heads * rope) % LANES
    if short:
        w_qr = jnp.concatenate([w_qr, jnp.zeros((width, short), BF16)], axis=1)

    nz = n_sp // 4
    return pl.pallas_call(
        functools.partial(attention_kernel, n_sp, n_tp, heads, nope, rope, factor),
        out_shape=jax.ShapeDtypeStruct((rows, width), BF16),
        in_specs=[vmem] * 5 + [pl.BlockSpec(memory_space=pl.ANY)] * 5 + [vmem] * 2,
        out_specs=vmem,
        scratch_shapes=[
            pltpu.VMEM(w_qr.shape, BF16),
            pltpu.VMEM(w_qn.shape, BF16),
            pltpu.VMEM(w_key_up.shape, BF16),
            pltpu.VMEM(w_value_up.shape, BF16),
            pltpu.VMEM(w_out.shape, BF16),
            dma((5,)),
            pltpu.VMEM((n_tp, nz, 4 * period, rank + LANES), BF16),
            pltpu.VMEM((n_tp, rows, width), BF16),
            pltpu.VMEM((heads, tokens, nope + LANES), BF16),
            pltpu.VMEM((heads, tokens, nope), F32),
            pltpu.VMEM((heads, tokens, LANES), F32),
            pltpu.VMEM((heads, tokens, LANES), F32),
            pltpu.VMEM((tokens, heads * nope), BF16),
            pltpu.VMEM((n_tp, rows, width), BF16),
            pltpu.VMEM((n_tp, rows, width), BF16),
            dma((4, nz, 4)),
            dma((nz, 4)),
            dma((n_tp, nz, 4)),
            dma((n_tp, nz, 4)),
            dma((n_tp,)),
            dma((n_tp,)),
            dma((n_tp,)),
            dma((n_tp,)),
        ],
        compiler_params=pltpu.CompilerParams(
            collective_id=1, has_side_effects=True, vmem_limit_bytes=60 * 1024 * 1024
        ),
        name="attention",
    )(h, packed, bias, cosine, sine, w_qn, w_qr, w_key_up, w_value_up, w_out, latent, gate)


def solution(mesh):
    placed = (
        P(("sp", "tp"), None),
        P(),
        P(),
        P(("sp", "tp"), None),
        P("sp", "tp"),
        P("sp", "tp"),
        P("sp", "tp"),
        P(),
        P(None, "tp"),
        P(None, "tp"),
        P(),
        P(),
        P(),
        P(None, "tp"),
        P(None, "tp"),
        P("tp"),
        P("tp", None),
    )
    return jax.shard_map(
        body, mesh=mesh, in_specs=placed, out_specs=P(("sp", "tp"), None), check_vma=False
    )
```

```python
import functools

import jax
import jax.numpy as jnp
from jax import lax
from jax.experimental import pallas as pl
from jax.experimental.pallas import tpu as pltpu
from jax.sharding import PartitionSpec as P

GRID_W = 128
EPS = 1e-06
ROPE_BASE = 10000.0
LANES = 128
LOG2E = 1.4426950408889634
FLAGS = 4
MESH = pl.DeviceIdType.MESH
F32 = jnp.float32
BF16 = jnp.bfloat16


def remote(src, dst, send, recv, device):
    return pltpu.make_async_remote_copy(
        src_ref=src, dst_ref=dst, send_sem=send, recv_sem=recv, device_id=device, device_id_type=MESH
    )


def rotate(values, cosine, sine):
    width = values.shape[-1]
    ahead = pltpu.roll(values, width - 1, 1)
    behind = pltpu.roll(values, 1, 1)
    even = lax.broadcasted_iota(jnp.int32, values.shape, 1) % 2 == 0
    return values * cosine + jnp.where(even, ahead, behind) * sine


def modulation_kernel(
    n_sp, n_tp, rows, ctx_rows,
    pair_ref, shift_w, scale_w, gate_w, x_ref, gain_ref, down_ref, rope_ref, kv_gain_ref, cos_ref, sin_ref,
    h_ref, packed_ref, gate_ref,
    part, landed, reduced, full, mods, send1, recv1, send2, recv2,
):
    me = lax.axis_index("sp")
    mine = lax.axis_index("tp")
    total = n_sp * n_tp
    flat = me * n_tp + mine
    barrier = pltpu.get_barrier_semaphore()

    def greet(i, _):
        other = lax.rem(flat + i, total)
        pl.semaphore_signal(barrier, inc=1, device_id=(other // n_tp, other % n_tp), device_id_type=MESH)
        return 0

    lax.fori_loop(1, total, greet, 0)

    columns = shift_w.shape[1]
    blocks = columns // LANES
    per = -(-6 * blocks // n_sp)
    part[...] = jnp.zeros_like(part)
    pair = pair_ref[...]
    for which, weight in enumerate((shift_w, scale_w, gate_w)):
        product = jnp.dot(pair, weight[...], precision=lax.Precision.HIGHEST, preferred_element_type=F32)
        for row in range(2):
            for block in range(blocks):
                unit = (which * 2 + row) * blocks + block
                part[unit // per, unit % per : unit % per + 1, :] = product[
                    row : row + 1, block * LANES : (block + 1) * LANES
                ]
    pl.semaphore_wait(barrier, total - 1)

    def scatter(i, _):
        other = lax.rem(me + i, n_sp)
        remote(part.at[other], landed.at[me], send1.at[other], recv1.at[me], (other, mine)).start()
        return 0

    lax.fori_loop(1, n_sp, scatter, 0)
    landed[me] = part[me]

    def scattered(i, _):
        other = lax.rem(me + i, n_sp)
        remote(part.at[other], landed.at[other], send1.at[other], recv1.at[other], (other, mine)).wait()
        return 0

    lax.fori_loop(1, n_sp, scattered, 0)
    reduced[...] = jnp.sum(landed[...], axis=0)

    def gather(i, _):
        other = lax.rem(flat + i, total)
        remote(
            reduced, full.at[flat], send2.at[other], recv2.at[flat], (other // n_tp, other % n_tp)
        ).start()
        return 0

    lax.fori_loop(1, total, gather, 0)
    full[flat] = reduced[...]
    x = x_ref[...].astype(F32)
    normed = x * lax.rsqrt(jnp.mean(x * x, axis=-1, keepdims=True) + EPS) * gain_ref[...]

    def gathered(i, _):
        other = lax.rem(flat + i, total)
        remote(
            reduced, full.at[other], send2.at[other], recv2.at[other], (other // n_tp, other % n_tp)
        ).wait()
        return 0

    lax.fori_loop(1, total, gathered, 0)
    for unit in range(6 * blocks):
        row, block = unit // blocks, unit % blocks
        for t in range(n_tp):
            at = t * columns + block * LANES
            mods[row : row + 1, at : at + LANES] = full[(unit // per) * n_tp + t, unit % per : unit % per + 1, :]
    index = lax.broadcasted_iota(jnp.int32, (x.shape[0], 1), 0)
    latent_row = index < rows
    shift = jnp.where(latent_row, mods[0:1, :], mods[1:2, :])
    scale = jnp.where(latent_row, mods[2:3, :], mods[3:4, :])
    h = (normed * (1.0 + scale) + shift).astype(BF16)
    gate_ref[...] = mods[4:5, :]
    h_ref[...] = h[:rows]
    inner = jnp.dot(h, down_ref[...], preferred_element_type=F32)
    inner = inner * lax.rsqrt(jnp.mean(inner * inner, axis=-1, keepdims=True) + EPS)
    rank = inner.shape[1]
    packed_ref[:, :rank] = (inner * kv_gain_ref[...]).astype(BF16)
    rope = rope_ref.shape[1]
    key = jnp.dot(h, rope_ref[...], preferred_element_type=F32)
    key = jnp.concatenate([key, jnp.zeros((key.shape[0], LANES - rope), F32)], axis=1)
    key = rotate(key, cos_ref[...], sin_ref[...])
    lane = lax.broadcasted_iota(jnp.int32, key.shape, 1)
    is_ctx = (index >= rows) & (index < rows + ctx_rows)
    is_pad = index >= rows + ctx_rows
    flag = jnp.where(lane < rope + FLAGS - 1, is_ctx.astype(F32), is_pad.astype(F32))
    key = jnp.where(lane < rope, key, jnp.where(lane < rope + FLAGS, flag, 0.0))
    packed_ref[:, rank:] = key.astype(BF16)


def attention_kernel(
    n_sp, n_tp, heads, nope, rope, factor,
    h_ref, packed_ref, bias_ref, cos_ref, sin_ref, qn_hbm, qr_hbm, ku_hbm, vu_hbm, wo_hbm, latent_ref, gate_ref,
    out_ref,
    qr_ref, qn_ref, ku_ref, vu_ref, wo_ref, load_sem,
    buf, hbuf, q, acc, top, total, att, outbox, inbox, send, recv, send_t, recv_t, send_h, recv_h, send_o, recv_o,
):
    me = lax.axis_index("sp")
    mine = lax.axis_index("tp")
    loads = [
        pltpu.make_async_copy(src, dst, load_sem.at[i])
        for i, (src, dst) in enumerate(
            ((qr_hbm, qr_ref), (qn_hbm, qn_ref), (ku_hbm, ku_ref), (vu_hbm, vu_ref), (wo_hbm, wo_ref))
        )
    ]
    for load in loads:
        load.start()
    nz = n_sp // 4
    z, side = me // 4, me % 4
    y, x = side // 2, side % 2
    odd = mine % 2
    flip_x = y * 2 + (1 - x)
    flip_y = (1 - y) * 2 + x
    side_a = flip_x * (1 - odd) + flip_y * odd
    side_b = flip_y * (1 - odd) + flip_x * odd
    side_ab = 3 - side
    rows = h_ref.shape[0]
    period, width = packed_ref.shape
    rank = ku_ref.shape[0]

    def column_of(step, t):
        return lax.rem(z + step * (1 - 2 * (t % 2)) + 2 * nz, nz)

    def column(step):
        return column_of(step, mine)

    def peer(zz, ss):
        return (zz * 4 + ss, mine)

    ahead, back = peer(column(1), side), peer(column(-1), side)
    to_a, to_b = peer(z, side_a), peer(z, side_b)
    partners = [lax.rem(mine + i, n_tp) for i in range(1, n_tp)]

    barrier = pltpu.get_barrier_semaphore()
    for other in [ahead, back, to_a, to_b] + [(me, t) for t in partners]:
        pl.semaphore_signal(barrier, inc=1, device_id=other, device_id_type=MESH)
    pl.semaphore_wait(barrier, 3 + n_tp)

    def slot(zz, ss, t):
        return buf.at[t, zz, pl.ds(pl.multiple_of(ss * period, period), period)]

    started = []

    def link(step, ss, way, own, device):
        zz = column(step)
        src = packed_ref if own else slot(zz, ss, mine)
        return remote(src, slot(zz, ss, mine), send.at[way, zz, ss], recv.at[zz, ss], device)

    def over(step, ss, own, t):
        zz = column(step)
        src = packed_ref if own else slot(zz, ss, mine)
        return remote(src, slot(zz, ss, mine), send_t.at[t, zz, ss], recv_t.at[mine, zz, ss], (me, t))

    def push(step, ss, way, own, device):
        link(step, ss, way, own, device).start()
        started.append(lambda: link(step, ss, way, own, device))

    def across(step, ss, own=False):
        for t in partners:
            over(step, ss, own, t).start()
            started.append(lambda t=t: over(step, ss, own, t))

    def arrived(zz, ss):
        remote(slot(zz, ss, mine), slot(zz, ss, mine), send.at[0, zz, ss], recv.at[zz, ss], ahead).wait_recv()

    forward = nz // 2
    backward = nz - 1 - forward
    order = [0]
    for j in range(1, forward + 1):
        order.append(-j)
        if j <= backward:
            order.append(j)

    for t in partners:
        copy = remote(h_ref, hbuf.at[mine], send_h.at[t], recv_h.at[mine], (me, t))
        copy.start()
        started.append(lambda copy=copy: copy)

    def event_z(step):
        zz = column(step)
        own = step == 0
        if not own:
            arrived(zz, side)
        if own or (step < 0 and -step < forward):
            push(step, side, 0, own, ahead)
        if own or (step > 0 and step < backward):
            push(step, side, 1, own, back)
        push(step, side, 2, own, to_a)
        push(step, side, 3, own, to_b)
        across(step, side, own)

    def event_a(step):
        zz = column(step)
        arrived(zz, side_a)
        push(step, side_a, 3, False, to_b)
        across(step, side_a)

    def event_b(step, which):
        zz = column(step)
        arrived(zz, which)
        across(step, which)

    def ready(step):
        for t in partners:
            zz = column_of(step, t)
            for ss in (side, side_a, side_b, side_ab):
                remote(slot(zz, ss, t), slot(zz, ss, t), send_t.at[t, zz, ss], recv_t.at[t, zz, ss], (me, t)).wait_recv()

    event_z(0)
    hbuf[mine] = h_ref[...]
    buf[mine, z, pl.ds(pl.multiple_of(side * period, period), period), :] = packed_ref[...]
    acc[...] = jnp.zeros_like(acc)
    top[...] = jnp.full(top.shape, -1e38, F32)
    total[...] = jnp.zeros_like(total)
    for t in partners:
        remote(h_ref, hbuf.at[t], send_h.at[t], recv_h.at[t], (me, t)).wait_recv()

    tokens = n_tp * rows
    piece = hbuf[...].reshape(tokens, hbuf.shape[2])
    loads[0].wait()
    turned = jnp.dot(piece, qr_ref[...], preferred_element_type=F32)
    copies = turned.shape[1] // LANES
    turned = rotate(
        turned, jnp.concatenate([cos_ref[...]] * copies, axis=1), jnp.concatenate([sin_ref[...]] * copies, axis=1)
    ).astype(BF16)
    loads[1].wait()
    for head in range(heads):
        q[head, :, :nope] = jnp.dot(
            piece, qn_ref[:, head * nope : (head + 1) * nope], preferred_element_type=F32
        ).astype(BF16)
        q[head, :, nope : nope + rope] = turned[:, head * rope : (head + 1) * rope]
        q[head, :, nope + rope :] = jnp.broadcast_to(
            bias_ref[head : head + 1, :], (tokens, LANES - rope)
        )

    def attend(step, beside):
        places = [(t, column_of(step, t)) for t in range(n_tp)]

        def one(head, _):
            at = pl.ds(pl.multiple_of(head * nope, nope), nope)
            weight = jnp.concatenate([ku_ref[:, at], vu_ref[:, at]], axis=1)
            latents = jnp.concatenate([buf[t, zz, :, :rank] for t, zz in places], axis=0)
            extra = jnp.concatenate([buf[t, zz, :, rank:] for t, zz in places], axis=0)
            both = jnp.dot(latents, weight, preferred_element_type=F32).astype(BF16)
            keys = jnp.concatenate([both[:, :nope], extra], axis=1)
            scores = lax.dot_general(q[head], keys, (((1,), (1,)), ((), ())), preferred_element_type=F32)
            old = top[head][:, :1]
            new = jnp.maximum(old, jnp.max(scores, axis=-1, keepdims=True))
            weights = jnp.exp2((scores - new) * (factor * LOG2E))
            fade = jnp.exp2((old - new) * (factor * LOG2E))
            top[head] = jnp.broadcast_to(new, top.shape[1:])
            total[head] = total[head] * fade + jnp.sum(weights, axis=-1, keepdims=True)
            acc[head] = acc[head] * fade + jnp.dot(
                weights.astype(BF16), both[:, nope:], preferred_element_type=F32
            )
            return 0

        together = next(n for n in (4, 2, 1) if heads % n == 0)
        turns = heads // together

        def some(i, _):
            for k, event in enumerate(beside):
                pl.when(i == k * turns // len(beside))(event)
            for j in range(together):
                one(i * together + j, 0)
            return 0

        lax.fori_loop(0, turns, some, 0)

    event_a(0)
    event_z(order[1])
    event_b(0, side_b)
    event_b(0, side_ab)
    ready(0)
    loads[2].wait()
    loads[3].wait()
    for i, step in enumerate(order):
        if i + 1 < len(order):
            later = order[i + 1]
            attend(
                step,
                [
                    functools.partial(event_a, later),
                    functools.partial(event_b, later, side_b),
                    functools.partial(event_b, later, side_ab),
                ]
                + [functools.partial(event_z, step) for step in order[i + 2 : i + 3]],
            )
            ready(later)
        else:
            attend(step, [])
    loads[4].wait()

    for head in range(heads):
        att[:, head * nope : (head + 1) * nope] = (acc[head] / total[head]).astype(BF16)

    for t in partners:
        lines = pl.ds(pl.multiple_of(t * rows, rows), rows)
        outbox[t] = jnp.dot(att[lines, :], wo_ref[...], preferred_element_type=F32).astype(BF16)
        copy = remote(outbox.at[t], inbox.at[mine], send_o.at[t], recv_o.at[mine], (me, t))
        copy.start()
        started.append(lambda copy=copy: copy)
    lines = pl.ds(pl.multiple_of(mine * rows, rows), rows)
    branch = jnp.dot(att[lines, :], wo_ref[...], preferred_element_type=F32).astype(BF16).astype(F32)
    for t in partners:
        remote(outbox.at[t], inbox.at[t], send_o.at[t], recv_o.at[t], (me, t)).wait_recv()
        branch = branch + inbox[t].astype(F32)
    out_ref[...] = (latent_ref[...].astype(F32) + gate_ref[...] * branch).astype(BF16)
    for make in started:
        make().wait_send()


def tables(positions, rope, real):
    quarter = rope // 4
    lane = jnp.arange(LANES, dtype=jnp.int32)
    pair = (lane % rope) // 2
    inverse = ROPE_BASE ** (-(pair % quarter).astype(F32) / quarter)
    place = jnp.where(pair[None, :] < quarter, (positions // GRID_W)[:, None], (positions % GRID_W)[:, None])
    angle = jnp.where(real[:, None], place.astype(F32) * inverse[None, :], 0.0)
    sine = jnp.sin(angle)
    return jnp.cos(angle), jnp.where(lane[None, :] % 2 == 0, -sine, sine)


def body(
    latent, cond, ctx_mod, context, shift_w, scale_w, gate_w, norm_gain, w_qn, w_qr, w_kv_down, w_rope_key,
    kv_gain, w_key_up, w_value_up, ctx_bias, w_out,
):
    n_sp, n_tp = lax.axis_size("sp"), lax.axis_size("tp")
    sp_index, tp_index = lax.axis_index("sp"), lax.axis_index("tp")
    rows, width = latent.shape
    ctx_rows = context.shape[0]
    tokens = rows * n_tp
    heads = ctx_bias.shape[0]
    nope = w_key_up.shape[1] // heads
    rope = w_rope_key.shape[1]
    rank = w_kv_down.shape[1]
    period = -(-(rows + ctx_rows) // 16) * 16
    factor = (nope + rope) ** (-0.5)
    feat = shift_w.shape[0]
    pair = jnp.stack([jax.nn.silu(cond), jax.nn.silu(ctx_mod)])
    pair = lax.dynamic_slice_in_dim(pair, sp_index * feat, feat, 1)
    pair = jnp.concatenate([pair, jnp.zeros((6, feat), F32)], axis=0)
    pad = jnp.zeros((period - rows - ctx_rows, width), BF16)
    x = jnp.concatenate([latent, context, pad], axis=0)
    line = jnp.arange(period, dtype=jnp.int32)
    own_cos, own_sin = tables(sp_index * tokens + tp_index * rows + line, rope, line < rows)
    place = jnp.arange(tokens, dtype=jnp.int32)
    cosine, sine = tables(sp_index * tokens + place, rope, place >= 0)

    vmem = pl.BlockSpec(memory_space=pltpu.VMEM)
    dma = pltpu.SemaphoreType.DMA
    h, packed, gate = pl.pallas_call(
        functools.partial(modulation_kernel, n_sp, n_tp, rows, ctx_rows),
        out_shape=(
            jax.ShapeDtypeStruct((rows, width), BF16),
            jax.ShapeDtypeStruct((period, rank + LANES), BF16),
            jax.ShapeDtypeStruct((1, width), F32),
        ),
        in_specs=[vmem] * 11,
        out_specs=(vmem,) * 3,
        scratch_shapes=[
            pltpu.VMEM((n_sp, 8, LANES), F32),
            pltpu.VMEM((n_sp, 8, LANES), F32),
            pltpu.VMEM((8, LANES), F32),
            pltpu.VMEM((n_sp * n_tp, 8, LANES), F32),
            pltpu.VMEM((8, width), F32),
            dma((n_sp,)),
            dma((n_sp,)),
            dma((n_sp * n_tp,)),
            dma((n_sp * n_tp,)),
        ],
        compiler_params=pltpu.CompilerParams(
            collective_id=0, has_side_effects=True, vmem_limit_bytes=40 * 1024 * 1024
        ),
        name="modulation",
    )(
        pair, shift_w, scale_w, gate_w, x, norm_gain[None, :], w_kv_down, w_rope_key, kv_gain[None, :],
        own_cos, own_sin,
    )

    scaled = ctx_bias / factor
    high = lax.reduce_precision(scaled, 8, 7)
    middle = lax.reduce_precision(scaled - high, 8, 7)
    low = scaled - high - middle
    bias = jnp.stack([high, middle, low, jnp.full_like(scaled, -1e30)], axis=1)
    bias = jnp.concatenate([bias, jnp.zeros((heads, LANES - rope - FLAGS), F32)], axis=1).astype(BF16)
    short = -(heads * rope) % LANES
    if short:
        w_qr = jnp.concatenate([w_qr, jnp.zeros((width, short), BF16)], axis=1)

    nz = n_sp // 4
    return pl.pallas_call(
        functools.partial(attention_kernel, n_sp, n_tp, heads, nope, rope, factor),
        out_shape=jax.ShapeDtypeStruct((rows, width), BF16),
        in_specs=[vmem] * 5 + [pl.BlockSpec(memory_space=pl.ANY)] * 5 + [vmem] * 2,
        out_specs=vmem,
        scratch_shapes=[
            pltpu.VMEM(w_qr.shape, BF16),
            pltpu.VMEM(w_qn.shape, BF16),
            pltpu.VMEM(w_key_up.shape, BF16),
            pltpu.VMEM(w_value_up.shape, BF16),
            pltpu.VMEM(w_out.shape, BF16),
            dma((5,)),
            pltpu.VMEM((n_tp, nz, 4 * period, rank + LANES), BF16),
            pltpu.VMEM((n_tp, rows, width), BF16),
            pltpu.VMEM((heads, tokens, nope + LANES), BF16),
            pltpu.VMEM((heads, tokens, nope), F32),
            pltpu.VMEM((heads, tokens, LANES), F32),
            pltpu.VMEM((heads, tokens, LANES), F32),
            pltpu.VMEM((tokens, heads * nope), BF16),
            pltpu.VMEM((n_tp, rows, width), BF16),
            pltpu.VMEM((n_tp, rows, width), BF16),
            dma((4, nz, 4)),
            dma((nz, 4)),
            dma((n_tp, nz, 4)),
            dma((n_tp, nz, 4)),
            dma((n_tp,)),
            dma((n_tp,)),
            dma((n_tp,)),
            dma((n_tp,)),
        ],
        compiler_params=pltpu.CompilerParams(
            collective_id=1, has_side_effects=True, vmem_limit_bytes=60 * 1024 * 1024
        ),
        name="attention",
    )(h, packed, bias, cosine, sine, w_qn, w_qr, w_key_up, w_value_up, w_out, latent, gate)


def solution(mesh):
    placed = (
        P(("sp", "tp"), None),
        P(),
        P(),
        P(("sp", "tp"), None),
        P("sp", "tp"),
        P("sp", "tp"),
        P("sp", "tp"),
        P(),
        P(None, "tp"),
        P(None, "tp"),
        P(),
        P(),
        P(),
        P(None, "tp"),
        P(None, "tp"),
        P("tp"),
        P("tp", None),
    )
    return jax.shard_map(
        body, mesh=mesh, in_specs=placed, out_specs=P(("sp", "tp"), None), check_vma=False
    )
```
